32 devices in a mesh: ep: 8 (over z, y), tp: 4 (over x, core).
Axes of the slice: x: 2, y: 2, z: 4, core: 2. Of those that a mesh axis runs over, the one named last changes fastest.
Arguments:
- queries: bfloat16 [4096, 1536], P('ep', 'tp'), may hold values from -6 to 6
- keys: bfloat16 [4096, 1536], P('ep', 'tp'), may hold values from -6 to 6
- values: bfloat16 [4096, 1536], P('ep', 'tp'), may hold values from -6 to 6
- decay_gate_logits: float32 [4096, 12], P('ep', 'tp'), may hold values from -6 to 6
- correction_logits: bfloat16 [4096, 12], P('ep', 'tp'), may hold values from -6 to 6
- head_decay_speed: float32 [12], P('tp'), may hold values from 0 to 1
- position_log_decay: float32 [4096, 12], P('ep', 'tp'), may hold values from -1 to 0
- head_output_gain: float32 [128], replicated, may hold values from 0.1 to 1.9
- mixer_output_weight: bfloat16 [1536, 2048], P('tp'), may hold values from -0.15625 to 0.15625
- expert_input_tokens: bfloat16 [4096, 2048], P(('ep', 'tp')), may hold values from -6 to 6
- expert_norm_gain: float32 [2048], replicated, may hold values from 0.1 to 1.9
- routes: int32 [4096, 2], P(('ep', 'tp')), may hold values from 0 to 7, all different within a row; in each aligned block of 128 rows (0 to 127, 128 to 255, ...) at most 48 rows name the same one
- chosen_expert_weight: float32 [4096, 2], P(('ep', 'tp')), may hold values from 0.25 to 2.5
- routed_gate_weight: bfloat16 [8, 2048, 1024], P('ep', None, 'tp'), may hold values from -0.125 to 0.125
- routed_up_weight: bfloat16 [8, 2048, 1024], P('ep', None, 'tp'), may hold values from -0.125 to 0.125
- routed_down_weight: bfloat16 [8, 1024, 2048], P('ep', 'tp'), may hold values from -0.1875 to 0.1875
- common_gate_weight: bfloat16 [2048, 1024], P(None, 'tp'), may hold values from -0.125 to 0.125
- common_up_weight: bfloat16 [2048, 1024], P(None, 'tp'), may hold values from -0.125 to 0.125
- common_down_weight: bfloat16 [1024, 2048], P('tp'), may hold values from -0.1875 to 0.1875
Outputs:
- mixer_out: bfloat16 [4096, 2048], P(('ep', 'tp'))
- moe_out: bfloat16 [4096, 2048], P(('ep', 'tp'))
The draws below stay inside these ranges and needn't reach their ends.
Inputs may be any that keep to these rules, and one draw needn't show every extreme that they name: `routes`: each row names 2 different experts; the rows of one device name no expert more than 48 times, and some device names some expert exactly 48 times.
All inputs are finite; a program needn't handle non-finite values.
Results may differ from the reference program's by a relative error of at most 0.017.
Values may be sent and summed in bfloat16 or wider, within the bound.
A program may use at most 128 MiB of HBM per device.

```python
import math
import jax
import jax.numpy as jnp
import numpy as np
from jax import lax

D = 2048
HEADS = 12
HEAD_DIM = 128
BLOCK = 64
EXPERT_FF = 1024
SHARED_FF = 1024
TOP_K = 2
TOK_DEV = 128
EXPERTS = 8
CAP = 48
GROUP_ROWS = 512
TOKENS_A = 4096
TOKENS_B = 4096
N_EP = 8
N_TP = 4


def gentle_heads(key):
    order = jax.random.permutation(jax.random.fold_in(key, 41), HEADS)
    return order < max(1, HEADS // 4)


def draw_head_decay_speed(key, part):
    fast_share = 0.5
    gentle = gentle_heads(key)
    fast_head = (jax.random.uniform(jax.random.fold_in(key, 11), (HEADS,)) < fast_share) & jnp.logical_not(gentle)
    quick_rate = jax.random.uniform(jax.random.fold_in(key, 12), (HEADS,), jnp.float32, 0.02, 0.06)
    slow_rate = jax.random.uniform(jax.random.fold_in(key, 13), (HEADS,), jnp.float32, 0.5, 1.5) / TOKENS_A
    return jnp.where(fast_head, quick_rate, slow_rate).astype(jnp.float32)


def draw_correction_logits(key, part):
    gentle = gentle_heads(key)
    rough = jnp.clip(jax.random.normal(jax.random.fold_in(key, 42), (TOKENS_A, HEADS), jnp.float32), -6.0, 6.0)
    weak = jax.random.uniform(jax.random.fold_in(key, 43), (TOKENS_A, HEADS), jnp.float32, -6.0, -5.0)
    return jnp.where(gentle[None, :], weak, rough).astype(jnp.bfloat16)


def draw_position_log_decay(key, part):
    hit_draw = jax.random.uniform(jax.random.fold_in(key, 21), (TOKENS_A, HEADS))
    depth = jax.random.uniform(jax.random.fold_in(key, 22), (TOKENS_A, HEADS), jnp.float32, 0.5, 0.8)
    return jnp.where(hit_draw < 4.0 / TOKENS_A, jnp.log(depth), 0.0).astype(jnp.float32)


def draw_decay_gate_logits(key, part):
    lower_end = -1.5
    upper_end = 1.5
    base_draw = jax.random.normal(jax.random.fold_in(key, 31), (TOKENS_A, HEADS), jnp.float32)
    shifts = jax.random.uniform(jax.random.fold_in(key, 32), (TOKENS_A // GROUP_ROWS, 1), jnp.float32, lower_end, upper_end)
    owner = jnp.arange(TOKENS_A) // GROUP_ROWS
    return jnp.clip(base_draw + shifts[owner], -6.0, 6.0).astype(jnp.float32)


def block_scale(own_key, dims, split, low, top_value):
    def one(position, blocks):
        heights = jax.random.uniform(jax.random.fold_in(jax.random.fold_in(own_key, 6), position), (blocks,), jnp.float32, low / len(split), top_value / len(split))
        return jnp.repeat(jnp.exp(heights), dims[position] // blocks).reshape((-1,) + (1,) * (len(dims) - position - 1))

    gain = one(*split[0])
    for cut in split[1:]:
        gain = gain * one(*cut)
    return gain


def deal_out(key, own, number, rows, count, top, reach, skew):
    sequence = jax.random.permutation(key, count)
    heavy_load, common = portions_of(count, rows * top, reach, skew, True), portions_of(count, rows * top, reach, skew, False)
    places = jnp.arange(count)

    def named(sizes, offset_by):
        used = int((sizes > 0).sum())
        fixed = max(1, used // 4)
        moved = fixed + (places - fixed + offset_by * (used - fixed)) % max(1, count - fixed)
        return jnp.zeros((count,), jnp.int32).at[sequence[jnp.where(places < fixed, places, moved)]].set(jnp.asarray(sizes, jnp.int32))

    sizes = jnp.where(number % 4 == 0, named(heavy_load, number // 4), named(common, number - number // 4 - 1))
    mixed = jax.random.permutation(jax.random.fold_in(own, 3), count)
    giver, taker = mixed[0:count // 2 * 2:2], mixed[1:count // 2 * 2:2]
    margin = jnp.minimum(sizes[giver] - 1, reach - sizes[taker]) // 2
    margin = jnp.where((giver == sequence[0]) | (taker == sequence[0]) | (sizes[taker] == 0), 0, jnp.maximum(margin, 0))
    moved = jax.random.randint(jax.random.fold_in(own, 4), (count // 2,), 0, 1 << 20) % (margin + 1)
    sizes = sizes.at[giver].add(-moved).at[taker].add(moved)
    members = jnp.searchsorted(jnp.cumsum(sizes), jnp.arange(rows * top), side="right").astype(jnp.int32)
    grid = members.reshape(top, rows).T
    grid = grid[jax.random.permutation(jax.random.fold_in(own, 1), rows)]
    offset_by = jax.random.randint(jax.random.fold_in(own, 2), (rows, 1), 0, top)
    return jnp.take_along_axis(grid, (jnp.arange(top)[None, :] + offset_by) % top, axis=1)


def portions_of(amount, total, most, lean, full):
    loads = [(1 << 20) // math.isqrt(standing ** lean) + 1 for standing in range(1, amount + 1)]
    largest = most if full else min(most, max(-(-total // amount), total * loads[0] // sum(loads)))
    least = 1 if total - largest >= amount - 1 else 0
    counts, spare = [largest] + [least] * (amount - 1), total - largest - least * (amount - 1)
    while spare > 0:
        candidates = [i for i in range(1, amount) if counts[i] < largest] or [i for i in range(1, amount) if counts[i] < most]
        whole, budget = sum([loads[i] for i in candidates]), spare
        for i in candidates:
            addition = min(most - counts[i], max(1, budget * loads[i] // whole), spare)
            counts[i] = counts[i] + addition
            spare = spare - addition
    return np.array(counts)


def gaussian(rng, extent, deviation, bound, cuts=(), kind=jnp.bfloat16):
    array = jax.random.normal(rng, extent, jnp.float32) * deviation
    if len(cuts) > 0:
        array = block_scale(rng, extent, cuts, -0.22, 0.18) * array
    return jnp.clip(array, min=-bound, max=bound).astype(kind)


def setup_inputs(seed: int = 0) -> dict:
    seeds = jax.random.split(jax.random.key(seed), 20)
    queries = gaussian(seeds[0], (TOKENS_A, HEADS * HEAD_DIM), 1.0, 6.0, ((0, 8), (1, 4)))
    keys = gaussian(seeds[1], (TOKENS_A, HEADS * HEAD_DIM), 1.0, 6.0, ((0, 8), (1, 4)))
    values = gaussian(seeds[2], (TOKENS_A, HEADS * HEAD_DIM), 1.0, 6.0, ((0, 8), (1, 4)))
    decay_gate_logits = draw_decay_gate_logits(jax.random.fold_in(seeds[19], 71), 0)
    correction_logits = draw_correction_logits(jax.random.fold_in(seeds[19], 71), 0)
    head_decay_speed = draw_head_decay_speed(jax.random.fold_in(seeds[19], 71), 0)
    position_log_decay = draw_position_log_decay(jax.random.fold_in(seeds[19], 71), 0)
    head_output_gain = jnp.clip(1.0 + 0.18 * jax.random.normal(seeds[7], (HEAD_DIM,), jnp.float32), 0.1, 1.9)
    mixer_output_weight = gaussian(seeds[8], (HEADS * HEAD_DIM, D), (HEADS * HEAD_DIM) ** -0.5, 0.15625, ((0, 4),))
    expert_input_tokens = gaussian(seeds[9], (TOKENS_B, D), 1.0, 6.0, ((0, 32),))
    expert_norm_gain = jnp.clip(1.0 + 0.18 * jax.random.normal(seeds[10], (D,), jnp.float32), 0.1, 1.9)
    routes_keys = jax.random.split(jax.random.fold_in(seeds[11], 1), TOKENS_B // TOK_DEV)
    routes_turns = jax.random.permutation(jax.random.fold_in(seeds[11], 3), TOKENS_B // TOK_DEV)
    routes = jax.vmap(lambda own, number: deal_out(jax.random.fold_in(seeds[11], 2), own, number, TOK_DEV, EXPERTS, TOP_K, CAP, 2))(routes_keys, routes_turns).reshape((TOKENS_B, TOP_K))
    chosen_expert_weight = jnp.clip(jnp.exp(math.log(2.5) - 2.3025851 * jax.random.uniform(seeds[12], (TOKENS_B, TOP_K), jnp.float32) ** block_scale(seeds[12], (TOKENS_B, TOP_K), ((0, 32),), -0.2, 0.2)), 0.25, 2.5)
    routed_gate_weight = gaussian(seeds[13], (EXPERTS, D, EXPERT_FF), D ** -0.5, 0.125, ((0, 8), (2, 4)))
    routed_up_weight = gaussian(seeds[14], (EXPERTS, D, EXPERT_FF), D ** -0.5, 0.125, ((0, 8), (2, 4)))
    routed_down_weight = gaussian(seeds[15], (EXPERTS, EXPERT_FF, D), EXPERT_FF ** -0.5, 0.1875, ((0, 8), (1, 4)))
    common_gate_weight = gaussian(seeds[16], (D, SHARED_FF), D ** -0.5, 0.125, ((1, 4),))
    common_up_weight = gaussian(seeds[17], (D, SHARED_FF), D ** -0.5, 0.125, ((1, 4),))
    common_down_weight = gaussian(seeds[18], (SHARED_FF, D), SHARED_FF ** -0.5, 0.1875, ((0, 4),))
    return {"queries": queries, "keys": keys, "values": values, "decay_gate_logits": decay_gate_logits, "correction_logits": correction_logits, "head_decay_speed": head_decay_speed, "position_log_decay": position_log_decay, "head_output_gain": head_output_gain, "mixer_output_weight": mixer_output_weight, "expert_input_tokens": expert_input_tokens, "expert_norm_gain": expert_norm_gain, "routes": routes, "chosen_expert_weight": chosen_expert_weight, "routed_gate_weight": routed_gate_weight, "routed_up_weight": routed_up_weight, "routed_down_weight": routed_down_weight, "common_gate_weight": common_gate_weight, "common_up_weight": common_up_weight, "common_down_weight": common_down_weight}


EPS = 1e-06
HIGH = lax.Precision.HIGHEST

def separate_heads(source, number_of_heads):
    row_count = source.shape[0]
    shaped = source.astype(jnp.float32).reshape(row_count // BLOCK, BLOCK, number_of_heads, source.shape[1] // number_of_heads)
    return jnp.transpose(shaped, (2, 0, 1, 3))

def block_contributions(queries, keys, values, decay_gate_logits, correction_logits, head_decay_speed, position_log_decay):
    number_of_heads = decay_gate_logits.shape[1]
    q_heads = separate_heads(queries, number_of_heads)
    k_heads = separate_heads(keys, number_of_heads)
    v_heads = separate_heads(values, number_of_heads)
    q_heads = q_heads * lax.rsqrt(lax.optimization_barrier(jnp.sum(q_heads * q_heads, axis=-1, keepdims=True)) + EPS) * q_heads.shape[-1] ** (-0.5)
    k_heads = k_heads * lax.rsqrt(lax.optimization_barrier(jnp.sum(k_heads * k_heads, axis=-1, keepdims=True)) + EPS)
    decay_speed_column = head_decay_speed.astype(jnp.float32)[:, None, None]
    log_gate_value = -decay_speed_column * jax.nn.softplus(separate_heads(decay_gate_logits, number_of_heads)[..., 0]) + separate_heads(position_log_decay, number_of_heads)[..., 0]
    beta_gate = jax.nn.sigmoid(separate_heads(correction_logits, number_of_heads)[..., 0])
    cum_gate = jnp.cumsum(log_gate_value, axis=-1)
    positions = jnp.arange(log_gate_value.shape[-1])
    causal = positions[:, None] >= positions[None, :]
    strict = positions[:, None] > positions[None, :]
    decay_mat = jnp.exp(jnp.where(causal, cum_gate[..., :, None] - cum_gate[..., None, :], -jnp.inf))
    keyed = k_heads * beta_gate[..., None]
    lower_part = jnp.where(strict, jnp.einsum('hnld,hnsd->hnls', keyed, k_heads, precision=HIGH) * decay_mat, 0.0)
    right_side = jnp.concatenate([v_heads * beta_gate[..., None], keyed * jnp.exp(cum_gate)[..., None]], axis=-1)
    solved = lax.linalg.triangular_solve(lower_part, right_side, left_side=True, lower=True, unit_diagonal=True)
    value_width = v_heads.shape[-1]
    new_values = solved[..., :value_width]
    corr_weights = solved[..., value_width:]
    scores = jnp.einsum('hnld,hnsd->hnls', q_heads, k_heads, precision=HIGH) * decay_mat
    carried_keys = k_heads * jnp.exp(cum_gate[..., -1:] - cum_gate)[..., None]
    q_scaled = q_heads * jnp.exp(cum_gate)[..., None]
    return (q_scaled, cum_gate[..., -1], scores, new_values, corr_weights, carried_keys)

def advance(state, inputs):
    q_blk, last_blk, score_blk, value_blk, weight_blk, carry_blk = inputs
    corrected = value_blk - jnp.einsum('hld,hde->hle', weight_blk, state, precision=HIGH)
    output = jnp.einsum('hld,hde->hle', q_blk, state, precision=HIGH) + jnp.einsum('hls,hse->hle', score_blk, corrected, precision=HIGH)
    state = state * jnp.exp(last_blk)[:, None, None] + jnp.einsum('hld,hle->hde', carry_blk, corrected, precision=HIGH)
    return (state, output)

def finish_heads(outputs, head_output_gain):
    normed = outputs * lax.rsqrt(lax.optimization_barrier(jnp.mean(outputs * outputs, axis=-1, keepdims=True)) + EPS) * head_output_gain.astype(jnp.float32)
    block_count, number_of_heads, span_len, value_width = normed.shape
    normed = jnp.transpose(normed, (0, 2, 1, 3)).reshape(block_count * span_len, number_of_heads * value_width)
    return normed.astype(jnp.bfloat16)

def norm_rows(expert_input_tokens, expert_norm_gain):
    rows_f = expert_input_tokens.astype(jnp.float32)
    scaled = rows_f * lax.rsqrt(lax.optimization_barrier(jnp.mean(rows_f * rows_f, axis=-1, keepdims=True)) + EPS) * expert_norm_gain.astype(jnp.float32)
    return scaled.astype(jnp.bfloat16)

def gated_hidden(rows_in, w_gate, w_up):
    gate_val = jnp.dot(rows_in.astype(jnp.float32), w_gate.astype(jnp.float32), preferred_element_type=jnp.float32)
    up_val = jnp.dot(rows_in.astype(jnp.float32), w_up.astype(jnp.float32), preferred_element_type=jnp.float32)
    return (jax.nn.silu(gate_val) * up_val).astype(jnp.bfloat16)

def mix_routes(chosen_expert_weight, copies, shared):
    running = shared
    for slot_k in range(chosen_expert_weight.shape[1]):
        running = running + chosen_expert_weight[:, slot_k:slot_k + 1] * copies[:, slot_k].astype(jnp.float32)
    return running.astype(jnp.bfloat16)

def reference(queries, keys, values, decay_gate_logits, correction_logits, head_decay_speed, position_log_decay, head_output_gain, mixer_output_weight, expert_input_tokens, expert_norm_gain, routes, chosen_expert_weight, routed_gate_weight, routed_up_weight, routed_down_weight, common_gate_weight, common_up_weight, common_down_weight):
    summands = block_contributions(queries, keys, values, decay_gate_logits, correction_logits, head_decay_speed, position_log_decay)
    number_of_heads = summands[0].shape[0]
    key_width = summands[0].shape[-1]
    value_width = summands[3].shape[-1]
    inputs = tuple((jnp.moveaxis(item, 1, 0) for item in summands))
    zero_state = jnp.zeros((number_of_heads, key_width, value_width), jnp.float32)
    _, outputs = lax.scan(advance, zero_state, inputs)
    normed = finish_heads(outputs, head_output_gain)
    part_width = HEADS // N_TP * HEAD_DIM
    running = jnp.zeros((normed.shape[0], mixer_output_weight.shape[1]), jnp.float32)
    for member in range(N_TP):
        part_sum = jnp.dot(normed[:, member * part_width:(member + 1) * part_width].astype(jnp.float32), mixer_output_weight[member * part_width:(member + 1) * part_width].astype(jnp.float32), preferred_element_type=jnp.float32).astype(jnp.bfloat16)
        running = running + part_sum.astype(jnp.float32)
    mixer_out = running.astype(jnp.bfloat16)
    normed_in = norm_rows(expert_input_tokens, expert_norm_gain)
    token_count, top_k = routes.shape
    flat_routes = routes.reshape(-1).astype(jnp.int32)
    copy_count = flat_routes.shape[0]
    row_limit = N_EP * N_TP * CAP
    unit_width = EXPERT_FF // N_TP

    def one_expert(results, expert):
        chosen = flat_routes == expert
        before = jnp.cumsum(chosen.astype(jnp.int32)) - 1
        target = jnp.where(chosen, before, row_limit).astype(jnp.int32)
        owners = jnp.zeros((row_limit + 1,), jnp.int32).at[target].set(jnp.arange(copy_count, dtype=jnp.int32))
        in_use = jnp.arange(row_limit, dtype=jnp.int32) < jnp.sum(chosen.astype(jnp.int32))
        picked = owners[:row_limit]
        picked_rows = normed_in[(picked // top_k).astype(jnp.int32)]
        hidden = gated_hidden(picked_rows, routed_gate_weight[expert], routed_up_weight[expert])
        running_e = jnp.zeros((row_limit, normed_in.shape[1]), jnp.float32)
        for member in range(N_TP):
            part_sum = jnp.dot(hidden[:, member * unit_width:(member + 1) * unit_width].astype(jnp.float32), routed_down_weight[expert, member * unit_width:(member + 1) * unit_width].astype(jnp.float32), preferred_element_type=jnp.float32).astype(jnp.bfloat16)
            running_e = running_e + part_sum.astype(jnp.float32)
        result = running_e.astype(jnp.bfloat16)
        spots = jnp.where(in_use, picked, copy_count).astype(jnp.int32)
        results = results.at[spots].set(result, mode='drop')
        return (results, None)
    start_rows = jnp.zeros((copy_count, normed_in.shape[1]), jnp.bfloat16)
    copies, _ = lax.scan(one_expert, start_rows, jnp.arange(EXPERTS, dtype=jnp.int32))
    shared_hidden = gated_hidden(normed_in, common_gate_weight, common_up_weight)
    shared_width = SHARED_FF // N_TP
    shared = jnp.zeros((token_count, normed_in.shape[1]), jnp.float32)
    for member in range(N_TP):
        part_sum = jnp.dot(shared_hidden[:, member * shared_width:(member + 1) * shared_width].astype(jnp.float32), common_down_weight[member * shared_width:(member + 1) * shared_width].astype(jnp.float32), preferred_element_type=jnp.float32).astype(jnp.bfloat16)
        shared = shared + part_sum.astype(jnp.float32)
    moe_out = mix_routes(chosen_expert_weight, copies.reshape(token_count, top_k, -1), shared)
    return (mixer_out, moe_out)
```

```python
import jax
import jax.numpy as jnp
from jax import lax
from jax.experimental import pallas as pl
from jax.experimental.pallas import tpu as pltpu
from jax.sharding import PartitionSpec as P


EPS = 1e-06


SPAN = 64


def halves(x):
    high = x.astype(jnp.bfloat16)
    return high, (x - high.astype(jnp.float32)).astype(jnp.bfloat16)


def product(left, right, numbers):
    left_high, left_low = halves(left)
    right_high, right_low = halves(right)

    def dot(x, y):
        return lax.dot_general(x, y, numbers, preferred_element_type=jnp.float32)

    return dot(left_high, right_high) + (dot(left_high, right_low) + dot(left_low, right_high))


def bmm(left, right, dims):
    return product(left, right, (dims, ((0,), (0,))))


def mm(left, right):
    return product(left, right, (((1,), (0,)), ((), ())))


def unit_lower_inverse(lower, rows, cols):
    inverse = jnp.where(rows == cols, 1.0, 0.0) - jnp.where(
        ((rows >> 1) == (cols >> 1)), lower, 0.0
    )
    level = 1
    while (1 << level) < SPAN:
        below = ((rows >> (level + 1)) == (cols >> (level + 1))) & (
            (rows >> level) != (cols >> level)
        )
        part = jnp.where(below, lower, 0.0)
        inverse = inverse - bmm(bmm(inverse, part, ((2,), (1,))), inverse, ((2,), (1,)))
        level += 1
    return inverse


def local_kernel(q_ref, k_ref, v_ref, ccol_ref, crow_ref, bcol_ref, g_ref, z_ref, total_ref):
    width = q_ref.shape[1]
    count = q_ref.shape[0] // SPAN
    shape = (count, SPAN, width)
    q = q_ref[...].astype(jnp.float32)
    k = k_ref[...].astype(jnp.float32)
    v = v_ref[...].astype(jnp.float32).reshape(shape)
    q = q * lax.rsqrt(jnp.sum(q * q, axis=-1, keepdims=True) + EPS) * width ** (-0.5)
    k = k * lax.rsqrt(jnp.sum(k * k, axis=-1, keepdims=True) + EPS)
    q = q.reshape(shape)
    k = k.reshape(shape)
    ccol = ccol_ref[0].reshape(count, SPAN, 1)
    crow = crow_ref[0]
    bcol = bcol_ref[0].reshape(count, SPAN, 1)
    rows = lax.broadcasted_iota(jnp.int32, (count, SPAN, SPAN), 1)
    cols = lax.broadcasted_iota(jnp.int32, (count, SPAN, SPAN), 2)
    decay = jnp.exp(jnp.where(rows >= cols, ccol - crow, -jnp.inf))
    keyed = k * bcol
    lower = jnp.where(rows > cols, bmm(keyed, k, ((2,), (2,))) * decay, 0.0)
    inverse = unit_lower_inverse(lower, rows, cols)
    grown = jnp.exp(ccol)
    solved = bmm(
        inverse, jnp.concatenate([keyed * grown, v * bcol], axis=-1), ((2,), (1,))
    )
    scores = bmm(q, k, ((2,), (2,))) * decay
    q_scaled = q * grown
    last = ccol[:, SPAN - 1 :, :]
    carried = k * jnp.exp(last - ccol)
    mixed = bmm(scores, solved, ((2,), (1,)))
    readout = q_scaled - mixed[:, :, :width]
    eye_r = lax.broadcasted_iota(jnp.int32, (width, width), 0)
    eye_c = lax.broadcasted_iota(jnp.int32, (width, width), 1)
    eye = jnp.where(eye_r == eye_c, 1.0, 0.0)
    state = jnp.concatenate([eye, jnp.zeros_like(eye)], axis=1)
    for n in range(count):
        seen = mm(readout[n], state)
        g_ref[0, n * SPAN : (n + 1) * SPAN, :] = seen[:, :width]
        z_ref[0, n * SPAN : (n + 1) * SPAN, :] = seen[:, width:] + mixed[n][:, width:]
        both = mm(carried[n].T, solved[n])
        trans = jnp.exp(last[n]) * eye - both[:, :width]
        state = mm(trans, state)
        state = jnp.concatenate([state[:, :width], state[:, width:] + both[:, width:]], axis=1)
    total_ref[0] = state.astype(jnp.bfloat16)


def finish_kernel(place_ref, gathered_ref, g_ref, z_ref, gain_ref, out_ref):
    width = g_ref.shape[2]

    def one(turn, state):
        both = gathered_ref[turn, 0].astype(jnp.float32)
        return mm(both[:, :width], state) + both[:, width:]

    state = lax.fori_loop(0, place_ref[0], one, jnp.zeros((width, width), jnp.float32))
    out = mm(g_ref[0], state) + z_ref[0]
    out = out * lax.rsqrt(jnp.mean(out * out, axis=-1, keepdims=True) + EPS) * gain_ref[...]
    out_ref[...] = out.astype(jnp.bfloat16)


def token_mixer_heads(
    queries,
    keys,
    values,
    decay_gate_logits,
    correction_logits,
    head_decay_speed,
    position_log_decay,
    head_output_gain,
):
    heads = decay_gate_logits.shape[1]
    length = queries.shape[0]
    width = queries.shape[1] // heads
    count = length // SPAN
    log_gate = -head_decay_speed * jax.nn.softplus(decay_gate_logits) + position_log_decay
    log_gate = log_gate.T.reshape(heads, count, SPAN)
    at = jnp.arange(SPAN)
    cum = jnp.sum(
        jnp.where(at[:, None] >= at[None, :], log_gate[:, :, None, :], 0.0), axis=-1
    )
    beta = jax.nn.sigmoid(correction_logits.astype(jnp.float32)).T.reshape(heads, length, 1)
    by_head = pl.BlockSpec((length, width), lambda h: (0, h))
    column = pl.BlockSpec((1, length, 1), lambda h: (h, 0, 0))
    whole = pl.BlockSpec((1, length, width), lambda h: (h, 0, 0))
    local_call = pl.pallas_call(
        local_kernel,
        grid=(heads,),
        in_specs=[
            by_head,
            by_head,
            by_head,
            column,
            pl.BlockSpec((1, count, 1, SPAN), lambda h: (h, 0, 0, 0)),
            column,
        ],
        out_specs=[whole, whole, pl.BlockSpec((1, width, 2 * width), lambda h: (h, 0, 0))],
        out_shape=[
            jax.ShapeDtypeStruct((heads, length, width), jnp.float32),
            jax.ShapeDtypeStruct((heads, length, width), jnp.float32),
            jax.ShapeDtypeStruct((heads, width, 2 * width), jnp.bfloat16),
        ],
        cost_estimate=pl.CostEstimate(
            flops=3_000_000_000, bytes_accessed=4_000_000, transcendentals=200_000
        ),
    )
    readout, local_out, total = local_call(
        queries,
        keys,
        values,
        cum.reshape(heads, length, 1),
        cum.reshape(heads, count, 1, SPAN),
        beta,
    )
    gathered = lax.all_gather(total, "ep")
    place = lax.axis_index("ep").astype(jnp.int32).reshape(1)
    devices = gathered.shape[0]
    return pl.pallas_call(
        finish_kernel,
        grid=(heads,),
        in_specs=[
            pl.BlockSpec(memory_space=pltpu.SMEM),
            pl.BlockSpec((devices, 1, width, 2 * width), lambda h: (0, h, 0, 0)),
            whole,
            whole,
            pl.BlockSpec((1, width), lambda h: (0, 0)),
        ],
        out_specs=by_head,
        out_shape=jax.ShapeDtypeStruct((length, heads * width), jnp.bfloat16),
        cost_estimate=pl.CostEstimate(
            flops=500_000_000, bytes_accessed=4_000_000, transcendentals=2_000
        ),
    )(place, gathered, readout, local_out, head_output_gain.reshape(1, width))


def norm_rows(expert_input_tokens, expert_norm_gain):
    rows_f = expert_input_tokens.astype(jnp.float32)
    scaled = (
        rows_f
        * lax.rsqrt(jnp.mean(rows_f * rows_f, axis=-1, keepdims=True) + EPS)
        * expert_norm_gain
    )
    return scaled.astype(jnp.bfloat16)


def gated_hidden(rows_in, w_gate, w_up):
    gate_val = jnp.dot(rows_in, w_gate, preferred_element_type=jnp.float32)
    up_val = jnp.dot(rows_in, w_up, preferred_element_type=jnp.float32)
    return (jax.nn.silu(gate_val) * up_val).astype(jnp.bfloat16)


def slot_layout(routes, capacity):
    flat = routes.reshape(-1)
    at = jnp.arange(flat.shape[0], dtype=jnp.int32)
    same = (flat[:, None] == flat[None, :]) & (at[None, :] < at[:, None])
    before = jnp.sum(same.astype(jnp.int32), axis=1)
    return (flat * capacity + before).reshape(routes.shape)


def shards(
    queries,
    keys,
    values,
    decay_gate_logits,
    correction_logits,
    head_decay_speed,
    position_log_decay,
    head_output_gain,
    mixer_output_weight,
    expert_input_tokens,
    expert_norm_gain,
    routes,
    chosen_expert_weight,
    routed_gate_weight,
    routed_up_weight,
    routed_down_weight,
    common_gate_weight,
    common_up_weight,
    common_down_weight,
):
    normed = token_mixer_heads(
        queries,
        keys,
        values,
        decay_gate_logits,
        correction_logits,
        head_decay_speed,
        position_log_decay,
        head_output_gain,
    )
    mixer_out = lax.psum_scatter(
        jnp.dot(normed, mixer_output_weight, preferred_element_type=jnp.float32).astype(
            jnp.bfloat16
        ),
        "tp",
        scatter_dimension=0,
        tiled=True,
    )
    normed_in = norm_rows(expert_input_tokens, expert_norm_gain)
    tokens_own, top_k = routes.shape
    model_width = expert_input_tokens.shape[1]
    experts = lax.axis_size("ep")
    capacity = 3 * tokens_own * top_k // (2 * experts)
    slot_count = experts * capacity
    slots = slot_layout(routes, capacity)
    numbers = jnp.arange(slot_count, dtype=jnp.int32)
    sends = sum(
        (slots[None, :, k] == numbers[:, None]).astype(jnp.bfloat16) for k in range(top_k)
    )
    outgoing = jnp.dot(sends, normed_in, preferred_element_type=jnp.float32).astype(
        jnp.bfloat16
    )
    arrived = lax.all_to_all(
        outgoing.reshape(experts, capacity, model_width),
        "ep",
        split_axis=0,
        concat_axis=0,
        tiled=True,
    ).reshape(slot_count, model_width)
    gate_all = lax.all_gather(routed_gate_weight[0], "tp")
    up_all = lax.all_gather(routed_up_weight[0], "tp")
    down_all = lax.all_gather(routed_down_weight[0], "tp", axis=0, tiled=True)
    hidden = jnp.concatenate(
        [gated_hidden(arrived, gate_all[t], up_all[t]) for t in range(gate_all.shape[0])],
        axis=1,
    )
    slot_sums = jnp.dot(hidden, down_all, preferred_element_type=jnp.float32).astype(
        jnp.bfloat16
    )
    returned = lax.all_to_all(
        slot_sums.reshape(experts, capacity, model_width),
        "ep",
        split_axis=0,
        concat_axis=0,
        tiled=True,
    ).reshape(slot_count, model_width)
    shared_hidden = gated_hidden(
        lax.all_gather(normed_in, "tp", axis=0, tiled=True), common_gate_weight, common_up_weight
    )
    shared = lax.psum_scatter(
        jnp.dot(shared_hidden, common_down_weight, preferred_element_type=jnp.float32).astype(
            jnp.bfloat16
        ),
        "tp",
        scatter_dimension=0,
        tiled=True,
    ).astype(jnp.float32)
    weights = sum(
        jnp.where(
            slots[:, k : k + 1] == numbers[None, :], chosen_expert_weight[:, k : k + 1], 0.0
        )
        for k in range(top_k)
    )
    coarse = weights.astype(jnp.bfloat16)
    fine = (weights - coarse.astype(jnp.float32)).astype(jnp.bfloat16)
    routed = jnp.dot(coarse, returned, preferred_element_type=jnp.float32) + jnp.dot(
        fine, returned, preferred_element_type=jnp.float32
    )
    moe_out = (shared + routed).astype(jnp.bfloat16)
    return (mixer_out, moe_out)


def solution(mesh):
    return jax.shard_map(
        shards,
        mesh=mesh,
        in_specs=(
            P("ep", "tp"),
            P("ep", "tp"),
            P("ep", "tp"),
            P("ep", "tp"),
            P("ep", "tp"),
            P("tp"),
            P("ep", "tp"),
            P(),
            P("tp", None),
            P(("ep", "tp"), None),
            P(),
            P(("ep", "tp"), None),
            P(("ep", "tp"), None),
            P("ep", None, "tp"),
            P("ep", None, "tp"),
            P("ep", "tp", None),
            P(None, "tp"),
            P(None, "tp"),
            P("tp", None),
        ),
        out_specs=(P(("ep", "tp"), None), P(("ep", "tp"), None)),
        check_vma=False,
    )
```
